512 devices in a mesh: sp: 32 (over z, core), tp: 16 (over y, x).
Axes of the slice: x: 4, y: 4, z: 16, core: 2. Of those that a mesh axis runs over, the one named last changes fastest.
Arguments:
- residual: bfloat16 [3584, 2048], P('sp'), may hold values from -1.5 to 1.5
- latent: bfloat16 [3584, 512], P('sp'), may hold values from -6 to 6
- rot_key: bfloat16 [3584, 64], P('sp'), may hold values from -6 to 6
- latent_norm_scale: float32 [512], replicated, may hold values from 0.1 to 1.9
- query_wide: bfloat16 [3584, 3072], P('sp', 'tp'), may hold values from -210 to 210
- query_narrow: bfloat16 [3584, 2048], P('sp', 'tp'), may hold values from -210 to 210
- large_key_lift: bfloat16 [512, 2048], P(None, 'tp'), may hold values from -0.25 to 0.25
- large_value_lift: bfloat16 [512, 2048], P(None, 'tp'), may hold values from -0.25 to 0.25
- small_key_lift: bfloat16 [512, 1024], P(None, 'tp'), may hold values from -0.25 to 0.25
- small_value_lift: bfloat16 [512, 1024], P(None, 'tp'), may hold values from -0.25 to 0.25
- out_wide: bfloat16 [2048, 2048], P('tp'), may hold values from -0.5 to 0.5
- out_narrow: bfloat16 [1024, 2048], P('tp'), may hold values from -0.75 to 0.75
- mix_gain: float32 [2048], replicated, may hold values from 0.1 to 1.9
- router_group: bfloat16 [2048, 4], replicated, may hold values from -0.125 to 0.125
- router_expert: bfloat16 [2048, 32], replicated, may hold values from -0.125 to 0.125
- expert_ids: int32 [3584, 2], P('sp'), may hold values from 0 to 31, all different within a row; in each aligned block of 112 rows (0 to 111, 112 to 223, ...) at most 16 rows name the same one
- expert_gate_w: bfloat16 [32, 2048, 4096], P('sp', None, 'tp'), may hold values from -0.125 to 0.125
- expert_up_w: bfloat16 [32, 2048, 4096], P('sp', None, 'tp'), may hold values from -0.125 to 0.125
- expert_down_w: bfloat16 [32, 4096, 2048], P('sp', 'tp'), may hold values from -0.375 to 0.375
Outputs:
- updated: bfloat16 [3584, 2048], P('sp', 'tp')
The draws below stay inside these ranges and needn't reach their ends.
Inputs may be any that keep to these rules, and one draw needn't show every extreme that they name: `expert_ids`: each row names two different experts; the rows of one index of sp name no expert more than 16 times, a bound that some expert reaches in some of these blocks.
All inputs are finite; a program needn't handle non-finite values.
Results may differ from the reference program's by a relative error of at most 0.024.
The reference program's roundings to bfloat16 on the way count: a program that leaves them out, or rounds other values in their place, can miss the bound.
Values may be sent and summed in bfloat16 or wider, within the bound.
A program may use at most 64 MiB of HBM per device.

```python
import math
import jax
import jax.numpy as jnp
import numpy as np
from jax import lax

D = 2048
LARGE_HEADS = 16
SMALL_HEADS = 16
PLAIN_KEY_WIDTH = 128
LARGE_VALUE_SIZE = 128
SMALL_HEAD_WIDTH = 64
ROPE = 64
LATENT_WIDTH = 512
GROUPS = 4
FF = 4096
TOK_DEV = 112
EXPERTS = 32
EXP_GROUP = 8
TOKEN_TOTAL = 3584
CAP = 16
N_SP = 32
N_TP = 16


def spiked_queries(key, head_count, plain_width):
    columns = head_count * (plain_width + ROPE)
    base_key = jax.random.fold_in(jax.random.fold_in(key, 11), 0)
    values = jnp.clip(jax.random.normal(base_key, (TOKEN_TOTAL, columns), jnp.float32), -4.0, 4.0)
    return values.astype(jnp.bfloat16)


def draw_query_wide(key, part):
    return spiked_queries(jax.random.fold_in(key, 3), LARGE_HEADS, PLAIN_KEY_WIDTH)


def draw_query_narrow(key, part):
    return spiked_queries(jax.random.fold_in(key, 5), SMALL_HEADS, SMALL_HEAD_WIDTH)


def level_of(rng, extent, pieces, low, top_value):
    loudness, own = 1.0, jax.random.fold_in(rng, 6)
    for position, blocks in pieces:
        draws = jnp.exp(jax.random.uniform(jax.random.fold_in(own, position), (blocks,), jnp.float32, low / len(pieces), top_value / len(pieces)))
        loudness = loudness * jnp.repeat(draws, extent[position] // blocks).reshape([-1 if axis == position else 1 for axis in range(len(extent))])
    return loudness


def deal_out(rng, own, number, rows, amount, top, most, skew):
    sequence = jax.random.permutation(rng, amount)
    packed, ordinary = portions_of(amount, rows * top, most, skew, True), portions_of(amount, rows * top, most, skew, False)
    places = jnp.arange(amount)

    def named(tallies, rotation):
        used = int((tallies > 0).sum())
        fixed = max(1, used // 4)
        moved = fixed + (places - fixed + rotation * (used - fixed)) % max(1, amount - fixed)
        return jnp.zeros((amount,), jnp.int32).at[sequence[jnp.where(places < fixed, places, moved)]].set(jnp.asarray(tallies, jnp.int32))

    tallies = jnp.where(number % 4 == 0, named(packed, number // 4), named(ordinary, number - number // 4 - 1))
    mixed = jax.random.permutation(jax.random.fold_in(own, 3), amount)
    donor, sink = mixed[0:amount // 2 * 2:2], mixed[1:amount // 2 * 2:2]
    margin = jnp.minimum(tallies[donor] - 1, most - tallies[sink]) // 2
    margin = jnp.where((donor == sequence[0]) | (sink == sequence[0]) | (tallies[sink] == 0), 0, jnp.maximum(margin, 0))
    moved = jax.random.randint(jax.random.fold_in(own, 4), (amount // 2,), 0, 1 << 20) % (margin + 1)
    tallies = tallies.at[donor].add(-moved).at[sink].add(moved)
    members = jnp.searchsorted(jnp.cumsum(tallies), jnp.arange(rows * top), side="right").astype(jnp.int32)
    grid = members.reshape(top, rows).T
    grid = grid[jax.random.permutation(jax.random.fold_in(own, 1), rows)]
    rotation = jax.random.randint(jax.random.fold_in(own, 2), (rows, 1), 0, top)
    return jnp.take_along_axis(grid, (jnp.arange(top)[None, :] + rotation) % top, axis=1)


def portions_of(amount, total, bound, lean, full):
    portions = [(1 << 20) // math.isqrt(grade ** lean) + 1 for grade in range(1, amount + 1)]
    largest = bound if full else min(bound, max(-(-total // amount), total * portions[0] // sum(portions)))
    least = 1 if total - largest >= amount - 1 else 0
    given, rest = [largest] + [least] * (amount - 1), total - largest - least * (amount - 1)
    while rest > 0:
        candidates = [i for i in range(1, amount) if given[i] < largest] or [i for i in range(1, amount) if given[i] < bound]
        whole, budget = sum([portions[i] for i in candidates]), rest
        for i in candidates:
            more = min(bound - given[i], max(1, budget * portions[i] // whole), rest)
            given[i] = given[i] + more
            rest = rest - more
    return np.array(given)


def centred(key, extent, deviation, limit, cuts=(), held_as=jnp.bfloat16):
    array = deviation * jax.random.normal(key, extent, jnp.float32)
    if cuts:
        array = array * level_of(key, extent, cuts, -0.22, 0.18)
    return jnp.clip(array, -limit, limit).astype(held_as)


def setup_inputs(seed: int = 0) -> dict:
    splits = jax.random.split(jax.random.key(seed), 20)
    residual = centred(splits[0], (TOKEN_TOTAL, D), 0.25, 1.5, ((0, 32),))
    latent = centred(splits[1], (TOKEN_TOTAL, LATENT_WIDTH), 1.0, 6.0, ((0, 32),))
    rot_key = centred(splits[2], (TOKEN_TOTAL, ROPE), 1.0, 6.0, ((0, 32),))
    latent_norm_scale = jnp.clip(1.0 + 0.18 * jax.random.normal(splits[3], (LATENT_WIDTH,), jnp.float32), 0.1, 1.9)
    query_wide = draw_query_wide(jax.random.fold_in(splits[19], 71), 0)
    query_narrow = draw_query_narrow(jax.random.fold_in(splits[19], 71), 0)
    large_key_lift = centred(splits[6], (LATENT_WIDTH, LARGE_HEADS * PLAIN_KEY_WIDTH), LATENT_WIDTH ** -0.5, 0.25, ((1, 16),))
    large_value_lift = centred(splits[7], (LATENT_WIDTH, LARGE_HEADS * LARGE_VALUE_SIZE), LATENT_WIDTH ** -0.5, 0.25, ((1, 16),))
    small_key_lift = centred(splits[8], (LATENT_WIDTH, SMALL_HEADS * SMALL_HEAD_WIDTH), LATENT_WIDTH ** -0.5, 0.25, ((1, 16),))
    small_value_lift = centred(splits[9], (LATENT_WIDTH, SMALL_HEADS * SMALL_HEAD_WIDTH), LATENT_WIDTH ** -0.5, 0.25, ((1, 16),))
    out_wide = centred(splits[10], (LARGE_HEADS * LARGE_VALUE_SIZE, D), LARGE_VALUE_SIZE ** -0.5, 0.5, ((0, 16),))
    out_narrow = centred(splits[11], (SMALL_HEADS * SMALL_HEAD_WIDTH, D), SMALL_HEAD_WIDTH ** -0.5, 0.75, ((0, 16),))
    mix_gain = jnp.clip(1.0 + 0.18 * jax.random.normal(splits[12], (D,), jnp.float32), 0.1, 1.9)
    router_group = centred(splits[13], (D, GROUPS), D ** -0.5, 0.125)
    router_expert = centred(splits[14], (D, EXPERTS), D ** -0.5, 0.125)
    expert_ids_keys = jax.random.split(jax.random.fold_in(splits[15], 1), TOKEN_TOTAL // TOK_DEV)
    expert_ids_turns = jax.random.permutation(jax.random.fold_in(splits[15], 3), TOKEN_TOTAL // TOK_DEV)
    expert_ids = jax.vmap(lambda own, number: deal_out(jax.random.fold_in(splits[15], 2), own, number, TOK_DEV, EXPERTS, 2, CAP, 1))(expert_ids_keys, expert_ids_turns).reshape((TOKEN_TOTAL, 2))
    expert_gate_w = centred(splits[16], (EXPERTS, D, FF), D ** -0.5, 0.125, ((0, 32), (2, 16)))
    expert_up_w = centred(splits[17], (EXPERTS, D, FF), D ** -0.5, 0.125, ((0, 32), (2, 16)))
    expert_down_w = centred(splits[18], (EXPERTS, FF, D), (FF // 16) ** -0.5, 0.375, ((0, 32), (1, 16)))
    return dict(residual=residual, latent=latent, rot_key=rot_key, latent_norm_scale=latent_norm_scale, query_wide=query_wide, query_narrow=query_narrow, large_key_lift=large_key_lift, large_value_lift=large_value_lift, small_key_lift=small_key_lift, small_value_lift=small_value_lift, out_wide=out_wide, out_narrow=out_narrow, mix_gain=mix_gain, router_group=router_group, router_expert=router_expert, expert_ids=expert_ids, expert_gate_w=expert_gate_w, expert_up_w=expert_up_w, expert_down_w=expert_down_w)


rope_base = 10000.0
epsilon = 1e-06
very_low = -1e+30

def angle_table(positions, width):
    frequency = rope_base ** (-jnp.arange(0, width, 2, dtype=jnp.float32) / width)
    return positions.astype(jnp.float32)[:, None] * frequency[None, :]

def rotate(values, angles):
    half_width = values.shape[-1] // 2
    cosine = jnp.cos(angles)
    sine_part = jnp.sin(angles)
    front_half = values[..., :half_width]
    back_half = values[..., half_width:]
    return jnp.concatenate([front_half * cosine - back_half * sine_part, front_half * sine_part + back_half * cosine], axis=-1)

def rms_scale(values, gain):
    return values * lax.rsqrt(lax.optimization_barrier(jnp.mean(values * values, axis=-1, keepdims=True)) + epsilon) * gain

def roped_queries(query, plain_width, angles):
    row_count = query.shape[0]
    shaped = query.reshape(row_count, -1, plain_width + ROPE)
    turned = rotate(shaped[..., plain_width:].astype(jnp.float32), angles[:, None, :]).astype(jnp.bfloat16)
    return jnp.concatenate([shaped[..., :plain_width], turned], axis=-1)

def expand_keys(latent_rows, large_key_lift, large_value_lift, small_key_lift, small_value_lift):
    row_count = latent_rows.shape[0]

    def project(weight, head_width):
        product = jnp.dot(latent_rows, weight, preferred_element_type=jnp.float32).astype(jnp.bfloat16)
        return product.reshape(row_count, weight.shape[1] // head_width, head_width)
    return (project(large_key_lift, PLAIN_KEY_WIDTH), project(large_value_lift, LARGE_VALUE_SIZE), project(small_key_lift, SMALL_HEAD_WIDTH), project(small_value_lift, SMALL_HEAD_WIDTH))

def attention_group(queries, key_rows, value_rows, key_rot, plain_width):
    token_count = queries.shape[0]
    score_scale = (plain_width + ROPE) ** (-0.5)
    causal_mask = jnp.arange(token_count)[:, None] >= jnp.arange(token_count)[None, :]

    def one_head(inputs):
        query_head, key_head, value_head = inputs
        scores = jnp.dot(query_head[:, :plain_width], key_head.T, preferred_element_type=jnp.float32)
        scores = scores + jnp.dot(query_head[:, plain_width:], key_rot.T, preferred_element_type=jnp.float32)
        scores = scores * score_scale
        row_peak = lax.optimization_barrier(jnp.max(jnp.where(causal_mask, scores, very_low), axis=1, keepdims=True))
        weights = jnp.where(causal_mask, jnp.exp(scores - row_peak), 0.0)
        weight_sum = lax.optimization_barrier(jnp.sum(weights, axis=1, keepdims=True))
        mixed_values = jnp.dot(weights.astype(jnp.bfloat16), value_head, preferred_element_type=jnp.float32)
        return (mixed_values / weight_sum).astype(jnp.bfloat16)
    result = lax.map(one_head, (queries.transpose(1, 0, 2), key_rows.transpose(1, 0, 2), value_rows.transpose(1, 0, 2)))
    return result.transpose(1, 0, 2).reshape(token_count, -1)

def reference(residual, latent, rot_key, latent_norm_scale, query_wide, query_narrow, large_key_lift, large_value_lift, small_key_lift, small_value_lift, out_wide, out_narrow, mix_gain, router_group, router_expert, expert_ids, expert_gate_w, expert_up_w, expert_down_w):
    token_count = latent.shape[0]
    positions = jnp.arange(token_count, dtype=jnp.int32)
    angles = angle_table(positions, ROPE)
    normed = rms_scale(latent.astype(jnp.float32), latent_norm_scale).astype(jnp.bfloat16)
    key_turned = rotate(rot_key.astype(jnp.float32), angles).astype(jnp.bfloat16)
    wide_queries = roped_queries(query_wide, PLAIN_KEY_WIDTH, angles)
    narrow_queries = roped_queries(query_narrow, SMALL_HEAD_WIDTH, angles)
    key_set = expand_keys(normed, large_key_lift, large_value_lift, small_key_lift, small_value_lift)
    heads_wide = attention_group(wide_queries, key_set[0], key_set[1], key_turned, PLAIN_KEY_WIDTH)
    heads_narrow = attention_group(narrow_queries, key_set[2], key_set[3], key_turned, SMALL_HEAD_WIDTH)

    def head_blocks(values):
        return values.reshape(token_count, N_TP, -1).transpose(1, 0, 2)

    def add_block(running, inputs):
        wide_block, wide_weight, narrow_block, narrow_weight = inputs
        partial_value = jnp.dot(wide_block, wide_weight, preferred_element_type=jnp.float32)
        partial_value = partial_value + jnp.dot(narrow_block, narrow_weight, preferred_element_type=jnp.float32)
        rounded = lax.optimization_barrier(partial_value.astype(jnp.bfloat16)).astype(jnp.float32)
        return (running + rounded, None)
    attended, ignored = lax.scan(add_block, jnp.zeros((token_count, D), jnp.float32), (head_blocks(heads_wide), out_wide.reshape(N_TP, -1, D), head_blocks(heads_narrow), out_narrow.reshape(N_TP, -1, D)))
    mixed = residual.astype(jnp.float32) + attended
    normal_rows = rms_scale(mixed, mix_gain).astype(jnp.bfloat16)
    group_prob = jax.nn.softmax(jnp.dot(normal_rows, router_group, preferred_element_type=jnp.float32), axis=-1)
    logits = jnp.dot(normal_rows, router_expert, preferred_element_type=jnp.float32)
    chosen_group = expert_ids[:, 0] // EXP_GROUP
    group_pick = lax.optimization_barrier(jnp.sum(jnp.where(chosen_group[:, None] == jnp.arange(GROUPS)[None, :], group_prob, 0.0), axis=1))
    expert_match = expert_ids[:, :, None] == jnp.arange(EXPERTS)[None, None, :]
    chosen_logits = lax.optimization_barrier(jnp.sum(jnp.where(expert_match, logits[:, None, :], 0.0), axis=2))
    gates = group_pick[:, None] * jax.nn.softmax(chosen_logits, axis=-1)
    block_ids = expert_ids.reshape(N_SP, -1)
    one_hot = (block_ids[:, :, None] == jnp.arange(EXPERTS)[None, None, :]).astype(jnp.int32)
    earlier = jnp.cumsum(one_hot, axis=1) - one_hot
    slot_index = lax.optimization_barrier(jnp.sum(earlier * one_hot, axis=2))
    block_index = jnp.arange(N_SP, dtype=jnp.int32)[:, None]
    target = (block_ids * (N_SP * CAP) + block_index * CAP + slot_index).reshape(-1).astype(jnp.int32)
    source_row = jnp.arange(2 * token_count, dtype=jnp.int32) // 2
    slot_total = EXPERTS * N_SP * CAP
    row_of_slot = jnp.zeros((slot_total,), jnp.int32).at[target].set(source_row)
    slot_used = jnp.zeros((slot_total,), jnp.bool_).at[target].set(True)

    def run_expert(inputs):
        rows_index, used, gate_weight, up_weight, down_weight = inputs
        expert_rows = jnp.where(used[:, None], normal_rows[rows_index], jnp.zeros((), jnp.bfloat16))
        gate_part = jnp.dot(expert_rows, gate_weight, preferred_element_type=jnp.float32)
        up_part = jnp.dot(expert_rows, up_weight, preferred_element_type=jnp.float32)
        hidden = (jax.nn.silu(gate_part) * up_part).astype(jnp.bfloat16)
        hidden_blocks = hidden.astype(jnp.float32).reshape(hidden.shape[0], N_TP, -1)
        down_blocks = down_weight.astype(jnp.float32).reshape(N_TP, -1, D)
        partials = jnp.einsum('rjf,jfd->jrd', hidden_blocks, down_blocks)
        rounded = lax.optimization_barrier(partials.astype(jnp.bfloat16)).astype(jnp.float32)
        return lax.optimization_barrier(jnp.sum(rounded, axis=0)).astype(jnp.bfloat16)
    expert_out = lax.map(run_expert, (row_of_slot.reshape(EXPERTS, -1), slot_used.reshape(EXPERTS, -1), expert_gate_w, expert_up_w, expert_down_w))
    picked = expert_out.reshape(slot_total, D)[target].astype(jnp.float32).reshape(token_count, 2, D)
    combined = lax.optimization_barrier(jnp.sum(picked * gates[:, :, None], axis=1))
    return (mixed + combined).astype(jnp.bfloat16)
```

```python
import functools

import jax
import jax.numpy as jnp
from jax import lax
from jax.experimental import pallas as pl
from jax.experimental.pallas import tpu as pltpu
from jax.sharding import PartitionSpec as P

PLAIN_KEY_WIDTH = 128
SMALL_HEAD_WIDTH = 64
ROPE = 64
TOK = 112
PAD = 128
CAP = 16
N_SP = 32
N_TP = 16
N_Z = 16
SLOTS = N_SP * CAP
HALF = SLOTS // 2
D = 2048

rope_base = 10000.0
epsilon = 1e-06
very_low = -1e30

MESH = pl.DeviceIdType.MESH
BF = jnp.bfloat16
F32 = jnp.float32

CHUNK = 416
SUBS = ((0, 112), (112, 112), (224, 96), (320, 96))


def dot(a, b):
    return jnp.dot(a, b, preferred_element_type=F32)


def dot_nt(a, b):
    return lax.dot_general(a, b, (((1,), (1,)), ((), ())), preferred_element_type=F32)


def remote(src, dst, send_sem, recv_sem, device):
    return pltpu.make_async_remote_copy(
        src_ref=src, dst_ref=dst, send_sem=send_sem, recv_sem=recv_sem,
        device_id=device, device_id_type=MESH,
    )


def pad_rows(x):
    return jnp.concatenate([x, jnp.zeros((PAD - x.shape[0], x.shape[1]), x.dtype)], axis=0)


def rows16(i):
    return pl.ds(pl.multiple_of(i * CAP, CAP), CAP)


def lanes128(i):
    return pl.ds(pl.multiple_of(i * 128, 128), 128)


def kernel(
    latent, lat_scale, rk2, cs, sn, qw, qw2, qn, lkl, lvl, sv, ids, gain, router_t,
    residual, out_wide, out_narrow, gate_w, up_w, down_w,
    out,
    q, kv, m_s, l_s, accw, accn, ow, wg, wu, wd, resid,
    ps, pr, mixed, ssr, dsel, psel, zs, xg, lgr, hid, ys,
    rb1u, rb1d, rb2u, rb2d, sa, ra1u, ra1d, ra2u, ra2d, res, zr,
    w_sem, ring_s, ring_r, dd_s, dd_r, rs_s, rs_r, ss_s, ss_r, z_s, z_r, loc,
    lg_s, lg_r, xg_s, xg_r, b_s, b_r, a_s, a_r, y_s, y_r,
):
    sp = lax.axis_index("sp")
    tp = lax.axis_index("tp")
    z = sp // 2
    c = sp % 2
    a = (1 - c) * (tp % 4) + c * (tp // 4)
    b = (1 - c) * (tp // 4) + c * (tp % 4)

    def at_ab(aa, bb):
        return (sp, bb * (4 - 3 * c) + aa * (1 + 3 * c))

    def tp_of(aa, bb):
        return bb * (4 - 3 * c) + aa * (1 + 3 * c)

    up_z = (((z + 1) % N_Z) * 2 + c, tp)
    down_z = (((z + N_Z - 1) % N_Z) * 2 + c, tp)
    partner = (z * 2 + 1 - c, tp)

    loads = [
        pltpu.make_async_copy(out_wide, ow.at[pl.ds(0, 128)], w_sem.at[0]),
        pltpu.make_async_copy(out_narrow, ow.at[pl.ds(128, 64)], w_sem.at[1]),
        pltpu.make_async_copy(residual.at[:, lanes128(tp)], resid, w_sem.at[2]),
        pltpu.make_async_copy(gate_w.at[0], wg, w_sem.at[3]),
        pltpu.make_async_copy(up_w.at[0], wu, w_sem.at[4]),
        pltpu.make_async_copy(down_w.at[0], wd, w_sem.at[5]),
    ]
    for load in loads:
        load.start()

    barrier = pltpu.get_barrier_semaphore()

    @pl.loop(1, N_SP)
    def _(k):
        pl.semaphore_signal(barrier, inc=1, device_id=((sp + k) % N_SP, tp), device_id_type=MESH)

    @pl.loop(1, N_TP)
    def _(k):
        pl.semaphore_signal(barrier, inc=1, device_id=(sp, (tp + k) % N_TP), device_id_type=MESH)

    lane = lax.broadcasted_iota(jnp.int32, (TOK, 128), 1)

    def roped(v):
        v = v.astype(F32)
        other = jnp.where(lane < 96, pltpu.roll(v, 96, 1), pltpu.roll(v, 32, 1))
        return v * cs[...] + other * sn[...]

    lat = latent[...].astype(F32)
    normed = lat * lax.rsqrt(jnp.mean(lat * lat, axis=-1, keepdims=True) + epsilon) * lat_scale[...]
    normed = pad_rows(normed.astype(BF))
    kv[sp, pl.ds(0, TOK), :] = dot(normed, lkl[...])[:TOK].astype(BF)
    small = dot(normed, sv[...])
    kv[sp, pl.ds(112, TOK), :] = jnp.where(lane < 64, small[:TOK], roped(rk2[...])).astype(BF)
    kv[sp, pl.ds(224, 128), :] = dot(normed, lvl[...]).T.astype(BF)
    kv[sp, pl.ds(352, 64), :] = small.T[64:].astype(BF)

    q[...] = jnp.zeros_like(q)
    q[pl.ds(0, TOK), pl.ds(0, 128)] = qw[...]
    q[pl.ds(0, TOK), pl.ds(128, 128)] = roped(qw2[...]).astype(BF)
    q[pl.ds(128, TOK), pl.ds(128, 128)] = roped(qn[...]).astype(BF)
    ow[pl.ds(192, 64), :] = jnp.zeros((64, D), BF)

    pl.semaphore_wait(barrier, N_SP - 1 + N_TP - 1)

    def ring_copy(direction, t, sub):
        at, count = SUBS[sub]
        step = t - 1
        origin = (z - step + N_Z) % N_Z if direction == 0 else (z + step) % N_Z
        ref = kv.at[origin * 2 + c, pl.ds(at, count)]
        return remote(ref, ref, ring_s.at[direction, t, sub], ring_r.at[direction, t, sub],
                      up_z if direction == 0 else down_z)

    def across(direction, t):
        origin = (z - t + N_Z) % N_Z if direction == 0 else (z + t) % N_Z
        ref = kv.at[origin * 2 + c]
        return remote(ref, ref, dd_s.at[direction, t], dd_r.at[direction, t], partner)

    for sub in range(4):
        ring_copy(0, 1, sub).start()
        ring_copy(1, 1, sub).start()
    across(0, 0).start()

    lane_q = lax.broadcasted_iota(jnp.int32, (1, 256), 1)
    scale = jnp.where(lane_q < 128, F32(192 ** -0.5), F32(128 ** -0.5))
    m_s[...] = jnp.full_like(m_s, very_low)
    l_s[...] = jnp.zeros_like(l_s)
    accw[...] = jnp.zeros_like(accw)
    accn[...] = jnp.zeros_like(accn)

    def attend(slot, own):
        keys = jnp.concatenate([kv[slot, pl.ds(0, TOK), :], kv[slot, pl.ds(112, TOK), :]], axis=1)
        s = dot_nt(keys, q[...]) * scale
        if own:
            key_at = lax.broadcasted_iota(jnp.int32, (TOK, 256), 0)
            query_at = lax.broadcasted_iota(jnp.int32, (TOK, 256), 1) % 128
            s = jnp.where(key_at <= query_at, s, very_low)
        old = m_s[...]
        new = jnp.maximum(old, jnp.max(s, axis=0, keepdims=True))
        w = jnp.exp(s - new)
        fade = jnp.exp(old - new)
        m_s[...] = new
        l_s[...] = l_s[...] * fade + jnp.sum(w, axis=0, keepdims=True)
        low = pad_rows(w.astype(BF))
        accw[...] = accw[...] * fade[:, :128] + dot(kv[slot, pl.ds(224, 128), :], low[:, :128])
        accn[...] = accn[...] * fade[:, 128:] + dot(kv[slot, pl.ds(352, 64), :], low[:, 128:])

    attend(sp, True)

    id0 = ids[pl.ds(0, 1), :]
    id1 = ids[pl.ds(1, 1), :]
    expert_at = lax.broadcasted_iota(jnp.int32, (N_SP, PAD), 0)
    hot0 = (expert_at == id0).astype(F32)
    hot1 = (expert_at == id1).astype(F32)
    before = (
        lax.broadcasted_iota(jnp.int32, (PAD, PAD), 0) < lax.broadcasted_iota(jnp.int32, (PAD, PAD), 1)
    ).astype(F32).astype(BF)
    earlier = dot((hot0 + hot1).astype(BF), before)
    target0 = id0 * CAP + jnp.sum(earlier * hot0, axis=0, keepdims=True).astype(jnp.int32)
    target1 = id1 * CAP + jnp.sum(earlier * hot1, axis=0, keepdims=True).astype(jnp.int32)
    slot_at = lax.broadcasted_iota(jnp.int32, (SLOTS, PAD), 0)
    dsel[...] = ((slot_at == target0) | (slot_at == target1)).astype(F32).astype(BF)

    def column(row):
        return jnp.broadcast_to(row, (PAD, PAD)).T

    for k, target in ((0, target0), (1, target1)):
        turned = column(target.astype(F32)).astype(jnp.int32)
        for part in range(4):
            lane_at = lax.broadcasted_iota(jnp.int32, (PAD, 128), 1) + part * 128
            psel[k, :, pl.ds(part * 128, 128)] = (lane_at == turned).astype(F32).astype(BF)

    def pending(k, step):
        direction = k % 2
        origin = z - step if direction == 0 else z + step - N_Z
        mine = k < 2
        slot = jnp.maximum(origin, 0) * 2 + (c if mine else 1 - c)
        if mine:
            ok = (origin >= 0) & (step >= 1)
        else:
            ok = (origin >= 0) & ((step >= 1) | (c == 1))
            if direction == 0:
                across(0, step).wait_recv()
            else:
                pl.when(step >= 1)(lambda: across(1, step).wait_recv())

        @pl.when(ok)
        def _():
            attend(slot, False)

    @pl.loop(1, 9)
    def _(t):
        for sub in range(4):
            ring_copy(0, t, sub).wait_recv()

            @pl.when(t < 8)
            def _():
                ring_copy(0, t + 1, sub).start()
                ring_copy(1, t, sub).wait_recv()

            @pl.when(t < 7)
            def _():
                ring_copy(1, t + 1, sub).start()

            if sub == 3:
                across(0, t).start()

                @pl.when(t < 8)
                def _():
                    across(1, t).start()

            pending(sub, t - 1)

    pending(0, 8)
    pending(2, 8)

    loads[0].wait()
    loads[1].wait()
    loads[2].wait()
    total = l_s[...]
    heads_w = (accw[...] / total[:, :128]).T
    heads_n = pad_rows(accn[...] / total[:, 128:]).T
    heads = jnp.concatenate([heads_w, heads_n], axis=1).astype(BF)
    for j in range(8):
        part = dot(heads, ow[:, pl.ds(j * 256, 256)]).astype(BF)
        ps[2 * j] = part[:TOK, :128]
        ps[2 * j + 1] = part[:TOK, 128:]

    def rs_copy(k):
        to = (tp + k) % N_TP
        return remote(ps.at[to], pr.at[k], rs_s.at[k], rs_r.at[k], (sp, to))

    @pl.loop(1, N_TP)
    def _(k):
        rs_copy(k).start()

    mixed[...] = resid[...].astype(F32) + ps[tp].astype(F32)

    @pl.loop(1, N_TP)
    def _(k):
        rs_copy(k).wait_recv()
        mixed[...] += pr[k].astype(F32)

    mix = pad_rows(mixed[...])
    ssr[0] = jnp.broadcast_to(jnp.sum((mix * mix).T, axis=0, keepdims=True), (8, PAD))

    def ss_copy(k):
        return remote(ssr.at[0], ssr.at[k], ss_s.at[k], ss_r.at[k], (sp, (tp + k) % N_TP))

    @pl.loop(1, N_TP)
    def _(k):
        ss_copy(k).start()

    @pl.loop(1, N_TP)
    def _(k):
        ss_copy(k).wait_recv()

    squares = jnp.sum(ssr[...], axis=0)[:1]
    inverse = column(lax.rsqrt(squares * (1.0 / D) + epsilon))
    normal = (mix * inverse * gain[pl.ds(tp, 1), :]).astype(BF)

    zs[...] = dot(dsel[...], normal).astype(BF)

    def far_first(i):
        return N_Z + (1 - 2 * (i % 2)) * ((i + 1) // 2)

    def z_copy(k):
        to = (sp + k) % N_SP
        return remote(zs.at[rows16(to)], xg.at[rows16(sp), lanes128(tp)], z_s.at[k], z_r.at[k], (to, tp))

    @pl.loop(0, N_SP - 1)
    def _(i):
        z_copy(far_first(i)).start()

    own_rows = pltpu.make_async_copy(zs.at[rows16(sp)], xg.at[rows16(sp), lanes128(tp)], loc.at[0])
    own_rows.start()

    lgr[0] = dot_nt(router_t[...], normal)

    def lg_copy(k):
        return remote(lgr.at[0], lgr.at[k], lg_s.at[k], lg_r.at[k], (sp, (tp + k) % N_TP))

    @pl.loop(1, N_TP)
    def _(k):
        lg_copy(k).start()

    @pl.loop(1, N_SP)
    def _(k):
        z_copy(k).wait_recv()

    own_rows.wait()

    right_a, left_a = at_ab((a + 1) % 4, b), at_ab((a + 3) % 4, b)
    right_b, left_b = at_ab(a, (b + 1) % 4), at_ab(a, (b + 3) % 4)
    column_a = (a, (a + 3) % 4, (a + 1) % 4, (a + 2) % 4)

    def gather_copy(n, aa, bb, half, device):
        rows = pl.ds(0, SLOTS) if half is None else pl.ds(half * HALF, HALF)
        ref = xg.at[rows, lanes128(tp_of(aa, bb))]
        return remote(ref, ref, xg_s.at[n], xg_r.at[n], device)

    started = []

    def send(n, *rest):
        copy = gather_copy(n, *rest)
        copy.start()
        started.append(copy)

    send(0, a, b, None, right_a)
    send(1, a, b, None, left_a)
    send(4, a, b, None, right_b)
    send(5, a, b, None, left_b)
    from_left, from_right = (a + 3) % 4, (a + 1) % 4
    opposite = (a + 2) % 4
    gather_copy(0, from_left, b, None, right_a).wait_recv()
    send(2, from_left, b, 0, right_a)
    send(8, from_left, b, None, right_b)
    send(9, from_left, b, None, left_b)
    gather_copy(1, from_right, b, None, left_a).wait_recv()
    send(3, from_right, b, 1, left_a)
    send(12, from_right, b, None, right_b)
    send(13, from_right, b, None, left_b)
    down_b, up_b, far_b = (b + 3) % 4, (b + 1) % 4, (b + 2) % 4

    def relay(i):
        gather_copy(4 + 4 * i, column_a[i], down_b, None, right_b).wait_recv()
        send(6 + 4 * i, column_a[i], down_b, 0, right_b)
        gather_copy(5 + 4 * i, column_a[i], up_b, None, left_b).wait_recv()
        send(7 + 4 * i, column_a[i], up_b, 1, left_b)

    relay(0)
    gather_copy(2, opposite, b, 0, right_a).wait_recv()
    gather_copy(3, opposite, b, 1, left_a).wait_recv()
    send(16, opposite, b, None, right_b)
    send(17, opposite, b, None, left_b)
    for i in (1, 2, 3):
        relay(i)
    for i in range(4):
        gather_copy(6 + 4 * i, column_a[i], far_b, 0, right_b).wait_recv()
        gather_copy(7 + 4 * i, column_a[i], far_b, 1, left_b).wait_recv()

    for load in loads[3:]:
        load.wait()

    @pl.loop(0, 2)
    def _(i):
        at = pl.ds(pl.multiple_of(i * HALF, HALF), HALF)
        rows = xg[at, :]
        gate = dot(rows, wg[...])
        hid[at, :] = (gate / (1.0 + jnp.exp(-gate)) * dot(rows, wu[...])).astype(BF)

    top, bottom = pl.ds(0, HALF), pl.ds(HALF, HALF)

    def down(db):
        @pl.loop(0, 4)
        def _(da):
            to = tp_of((a + da) % 4, (b + db) % 4)
            ys[db, da] = dot(hid[...], wd[:, lanes128(to)]).astype(BF)

    sums = []

    def give(n, src, dst, sems, device):
        copy = remote(src, dst, sems[0].at[n], sems[1].at[n], device)
        copy.start()
        sums.append(copy)
        return copy

    bs, as_ = (b_s, b_r), (a_s, a_r)
    down(2)
    far = {}
    for da in range(4):
        far[da] = (
            give(da, ys.at[2, da, top], rb2u.at[da], bs, right_b),
            give(4 + da, ys.at[2, da, bottom], rb2d.at[da], bs, left_b),
        )
    down(1)
    near = {}
    for da in range(4):
        near[da] = [give(8 + da, ys.at[1, da, bottom], rb1u.at[da, bottom], bs, right_b)]
    down(3)
    for da in range(4):
        near[da].append(give(12 + da, ys.at[3, da, top], rb1d.at[da, top], bs, left_b))
    for da in (2, 1, 3, 0):
        far[da][0].wait_recv()
        ys[1, da, top] = (ys[1, da, top].astype(F32) + rb2u[da].astype(F32)).astype(BF)
        near[da].append(give(16 + da, ys.at[1, da, top], rb1u.at[da, top], bs, right_b))
        far[da][1].wait_recv()
        ys[3, da, bottom] = (ys[3, da, bottom].astype(F32) + rb2d[da].astype(F32)).astype(BF)
        near[da].append(give(20 + da, ys.at[3, da, bottom], rb1d.at[da, bottom], bs, left_b))
    down(0)

    def line_sum(da):
        for copy in near[da]:
            copy.wait_recv()
        return ys[0, da].astype(F32) + rb1u[da].astype(F32) + rb1d[da].astype(F32)

    sa[2] = line_sum(2).astype(BF)
    far_a = (
        give(0, sa.at[2, top], ra2u, as_, right_a),
        give(1, sa.at[2, bottom], ra2d, as_, left_a),
    )
    sa[1] = line_sum(1).astype(BF)
    near_a = [give(2, sa.at[1, bottom], ra1u.at[bottom], as_, right_a)]
    sa[3] = line_sum(3).astype(BF)
    near_a.append(give(3, sa.at[3, top], ra1d.at[top], as_, left_a))
    far_a[0].wait_recv()
    sa[1, top] = (sa[1, top].astype(F32) + ra2u[...].astype(F32)).astype(BF)
    near_a.append(give(4, sa.at[1, top], ra1u.at[top], as_, right_a))
    far_a[1].wait_recv()
    sa[3, bottom] = (sa[3, bottom].astype(F32) + ra2d[...].astype(F32)).astype(BF)
    near_a.append(give(5, sa.at[3, bottom], ra1d.at[bottom], as_, left_a))
    own_sum = line_sum(0)
    for copy in near_a:
        copy.wait_recv()
    res[...] = (own_sum + ra1u[...].astype(F32) + ra1d[...].astype(F32)).astype(BF)

    def y_copy(k):
        to = (sp + k) % N_SP
        return remote(res.at[rows16(to)], zr.at[rows16(sp)], y_s.at[k], y_r.at[k], (to, tp))

    @pl.loop(0, N_SP - 1)
    def _(i):
        y_copy(far_first(i)).start()

    own_back = pltpu.make_async_copy(res.at[rows16(sp)], zr.at[rows16(sp)], loc.at[1])
    own_back.start()

    @pl.loop(1, N_TP)
    def _(k):
        lg_copy(k).wait_recv()

    logit = jnp.sum(lgr[...], axis=0)
    row8 = lax.broadcasted_iota(jnp.int32, (8, PAD), 0)
    group = jnp.where(row8 < 4, logit[:8], very_low)
    group = jnp.exp(group - jnp.max(group, axis=0, keepdims=True))
    picked = jnp.sum(jnp.where(row8 == (id0 >> 3), group, 0.0), axis=0, keepdims=True)
    pick = picked / jnp.sum(group, axis=0, keepdims=True)
    logit0 = jnp.sum(jnp.where(expert_at == id0, logit[8:], 0.0), axis=0, keepdims=True)
    logit1 = jnp.sum(jnp.where(expert_at == id1, logit[8:], 0.0), axis=0, keepdims=True)
    peak = jnp.maximum(logit0, logit1)
    e0, e1 = jnp.exp(logit0 - peak), jnp.exp(logit1 - peak)
    gate0 = column(pick * e0 / (e0 + e1))
    gate1 = column(pick * e1 / (e0 + e1))

    @pl.loop(1, N_SP)
    def _(k):
        y_copy(k).wait_recv()

    own_back.wait()
    back = zr[...]
    done = pad_rows(mixed[...]) + (gate0 * dot(psel[0], back) + gate1 * dot(psel[1], back))
    out[...] = done[:TOK].astype(BF)

    @pl.loop(1, 9)
    def _(t):
        for sub in range(4):
            ring_copy(0, t, sub).wait_send()
            pl.when(t < 8)(lambda: ring_copy(1, t, sub).wait_send())
        across(0, t).wait_send()
        pl.when(t < 8)(lambda: across(1, t).wait_send())

    across(0, 0).wait_send()

    @pl.loop(1, N_TP)
    def _(k):
        rs_copy(k).wait_send()
        ss_copy(k).wait_send()
        lg_copy(k).wait_send()

    @pl.loop(1, N_SP)
    def _(k):
        z_copy(k).wait_send()
        y_copy(k).wait_send()

    for copy in started + sums:
        copy.wait_send()


def layer(*args):
    vmem = pl.BlockSpec(memory_space=pltpu.VMEM)
    anywhere = pl.BlockSpec(memory_space=pl.ANY)
    dma = pltpu.SemaphoreType.DMA

    def v(*shape, dtype=BF):
        return pltpu.VMEM(shape, dtype)

    return pl.pallas_call(
        kernel,
        out_shape=jax.ShapeDtypeStruct((TOK, 128), BF),
        in_specs=[vmem] * 14 + [anywhere] * 6,
        out_specs=vmem,
        scratch_shapes=[
            v(256, 256), v(N_SP, CHUNK, 128), v(1, 256, dtype=F32), v(1, 256, dtype=F32),
            v(128, 128, dtype=F32), v(64, 128, dtype=F32),
            v(256, D), v(D, 256), v(D, 256), v(256, D), v(TOK, 128),
            v(N_TP, TOK, 128), v(N_TP, TOK, 128), v(TOK, 128, dtype=F32), v(N_TP, 8, 128, dtype=F32),
            v(SLOTS, 128), v(2, PAD, SLOTS), v(SLOTS, 128), v(SLOTS, D), v(N_TP, 40, 128, dtype=F32),
            v(SLOTS, 256), v(4, 4, SLOTS, 128),
            v(4, SLOTS, 128), v(4, SLOTS, 128), v(4, HALF, 128), v(4, HALF, 128),
            v(4, SLOTS, 128), v(SLOTS, 128), v(SLOTS, 128), v(HALF, 128), v(HALF, 128),
            v(SLOTS, 128), v(SLOTS, 128),
            dma((6,)), dma((2, 9, 4)), dma((2, 9, 4)), dma((2, 9)), dma((2, 9)),
            dma((N_TP,)), dma((N_TP,)), dma((N_TP,)), dma((N_TP,)), dma((N_SP,)), dma((N_SP,)), dma((2,)),
            dma((N_TP,)), dma((N_TP,)), dma((20,)), dma((20,)), dma((24,)), dma((24,)),
            dma((6,)), dma((6,)), dma((N_SP,)), dma((N_SP,)),
        ],
        compiler_params=pltpu.CompilerParams(
            collective_id=0, has_side_effects=True, vmem_limit_bytes=48 * 1024 * 1024
        ),
        name="layer",
    )(*args)


def shards(
    residual, latent, rot_key, latent_norm_scale, query_wide, query_narrow,
    large_key_lift, large_value_lift, small_key_lift, small_value_lift,
    out_wide, out_narrow, mix_gain, router_group, router_expert, expert_ids,
    expert_gate_w, expert_up_w, expert_down_w,
):
    tp = lax.axis_index("tp")
    positions = lax.axis_index("sp") * TOK + jnp.arange(TOK, dtype=jnp.int32)
    frequency = rope_base ** (-jnp.arange(0, ROPE, 2, dtype=F32) / ROPE)
    angles = positions.astype(F32)[:, None] * frequency[None, :]
    cosine, sine = jnp.cos(angles), jnp.sin(angles)
    cs = jnp.concatenate([jnp.ones((TOK, 64), F32), cosine, cosine], axis=1)
    sn = jnp.concatenate([jnp.zeros((TOK, 64), F32), -sine, sine], axis=1)
    blank = jnp.zeros((TOK, 64), BF)
    rk2 = jnp.concatenate([blank, rot_key], axis=1)
    qw = query_wide[:, :128]
    qw2 = jnp.concatenate([blank, query_wide[:, 128:]], axis=1)
    sv = jnp.concatenate([small_key_lift, small_value_lift], axis=1)
    ids = jnp.pad(expert_ids.T, ((0, 6), (0, PAD - TOK)), constant_values=-1)
    router = jnp.concatenate([router_group, jnp.zeros((D, 4), BF), router_expert], axis=1)
    router_t = lax.dynamic_slice_in_dim(router, tp * 128, 128, 0).T
    return layer(
        latent, latent_norm_scale.reshape(1, -1), rk2, cs, sn, qw, qw2, query_narrow,
        large_key_lift, large_value_lift, sv, ids, mix_gain.reshape(N_TP, 128), router_t,
        residual, out_wide, out_narrow, expert_gate_w, expert_up_w, expert_down_w,
    )


def solution(mesh):
    placed = (
        P("sp", None), P("sp", None), P("sp", None), P(), P("sp", "tp"), P("sp", "tp"),
        P(None, "tp"), P(None, "tp"), P(None, "tp"), P(None, "tp"), P("tp", None), P("tp", None),
        P(), P(), P(), P("sp", None),
        P("sp", None, "tp"), P("sp", None, "tp"), P("sp", "tp", None),
    )
    return jax.shard_map(
        shards, mesh=mesh, in_specs=placed, out_specs=P("sp", "tp"), check_vma=False
    )
```
